32 devices in a mesh: ep: 8 (over z, x), tp: 4 (over y, core).
Axes of the slice: x: 2, y: 2, z: 4, core: 2. Of those that a mesh axis runs over, the one named last changes fastest.
Arguments:
- hidden_in: bfloat16 [256, 2048], P('ep', 'tp'), may hold values from -6 to 6
- state_in: float32 [256, 8, 128, 128], P('ep', 'tp'), may hold values from -0.6 to 0.6
- attn_gain: float32 [2048], replicated, may hold values from 0.1 to 1.9
- w_query: bfloat16 [2048, 1024], P(None, 'tp'), may hold values from -0.125 to 0.125
- w_key: bfloat16 [2048, 1024], P(None, 'tp'), may hold values from -0.125 to 0.125
- w_value: bfloat16 [2048, 1024], P(None, 'tp'), may hold values from -0.125 to 0.125
- w_gate: bfloat16 [2048, 1024], P(None, 'tp'), may hold values from -0.125 to 0.125
- w_beta: bfloat16 [2048, 8], replicated, may hold values from -0.125 to 0.125
- w_decay: bfloat16 [2048, 8], replicated, may hold values from -0.125 to 0.125
- decay_scale: float32 [8], replicated, may hold values from 0.05 to 3
- head_gain: float32 [128], replicated, may hold values from 0.1 to 1.9
- w_output: bfloat16 [1024, 2048], P(None, 'tp'), may hold values from -0.1875 to 0.1875
- ffn_gain: float32 [2048], replicated, may hold values from 0.1 to 1.9
- expert_ids: int32 [256, 2], P('ep'), may hold values from 0 to 7, all different within a row; in each aligned block of 32 rows (0 to 31, 32 to 63, ...) at most 16 rows name the same one
- route_weight: float32 [256, 2], P('ep'), may hold values from 0.2 to 1
- expert_gate: bfloat16 [8, 2048, 3072], P('ep', None, 'tp'), may hold values from -0.125 to 0.125
- expert_up: bfloat16 [8, 2048, 3072], P('ep', None, 'tp'), may hold values from -0.125 to 0.125
- expert_down: bfloat16 [8, 3072, 2048], P('ep', 'tp'), may hold values from -0.109375 to 0.109375
- dense_gate: bfloat16 [2048, 4096], P(None, 'ep'), may hold values from -0.125 to 0.125
- dense_up: bfloat16 [2048, 4096], P(None, 'ep'), may hold values from -0.125 to 0.125
- dense_down: bfloat16 [4096, 2048], P('ep'), may hold values from -0.09375 to 0.09375
- dense_mix: float32 [2048], P('tp'), may hold values from -6 to 6
Outputs:
- result: bfloat16 [256, 2048], P('ep', 'tp')
- new_state: float32 [256, 8, 128, 128], P('ep', 'tp')
The draws below stay inside these ranges and needn't reach their ends.
Inputs may be any that keep to these rules, and one draw needn't show every extreme that they name: `expert_ids`: each row names 2 different experts. Within the rows of one index of ep (aligned blocks of 32 sequences) no expert is named more than 16 times, a bound that some block reaches.
All inputs are finite; a program needn't handle non-finite values.
Results may differ from the reference program's by a relative error of at most 0.015.
Values may be sent and summed in bfloat16 or wider, within the bound.
A program may use at most 64 MiB of HBM per device.

```python
import math
import jax
import jax.numpy as jnp
import numpy as np
from jax import lax

D = 2048
H = 8
DK = 128
DV = 128
FE = 3072
FFD = 4096
TOP = 2
SEQ_DEV = 32
EXPERTS = 8
CAP = 16
SEQS = 256
N_EP = 8
N_TP = 4


def steps_of(key, dims, shards, least, largest):
    def one(position, shards_of):
        heights = jax.random.uniform(jax.random.fold_in(jax.random.fold_in(key, 6), position), (shards_of,), jnp.float32, least / len(shards), largest / len(shards))
        return jnp.repeat(jnp.exp(heights), dims[position] // shards_of).reshape((-1,) + (1,) * (len(dims) - position - 1))

    level = one(*shards[0])
    for cut in shards[1:]:
        level = level * one(*cut)
    return level


def deal_out(key, own, number, rows, count, top, reach, skew):
    sequence = jax.random.permutation(key, count)
    packed, ordinary = portions_of(count, rows * top, reach, skew, True), portions_of(count, rows * top, reach, skew, False)
    places = jnp.arange(count)

    def named(lengths, offset_by):
        used = int((lengths > 0).sum())
        fixed = max(1, used // 4)
        shifted = fixed + (places - fixed + offset_by * (used - fixed)) % max(1, count - fixed)
        return jnp.zeros((count,), jnp.int32).at[sequence[jnp.where(places < fixed, places, shifted)]].set(jnp.asarray(lengths, jnp.int32))

    lengths = jnp.where(number % 4 == 0, named(packed, number // 4), named(ordinary, number - number // 4 - 1))
    mixed = jax.random.permutation(jax.random.fold_in(own, 3), count)
    donor, receiver = mixed[0:count // 2 * 2:2], mixed[1:count // 2 * 2:2]
    slack = jnp.minimum(lengths[donor] - 1, reach - lengths[receiver]) // 2
    slack = jnp.where((donor == sequence[0]) | (receiver == sequence[0]) | (lengths[receiver] == 0), 0, jnp.maximum(slack, 0))
    shifted = jax.random.randint(jax.random.fold_in(own, 4), (count // 2,), 0, 1 << 20) % (slack + 1)
    lengths = lengths.at[donor].add(-shifted).at[receiver].add(shifted)
    members = jnp.searchsorted(jnp.cumsum(lengths), jnp.arange(rows * top), side="right").astype(jnp.int32)
    listing = members.reshape(top, rows).T
    listing = listing[jax.random.permutation(jax.random.fold_in(own, 1), rows)]
    offset_by = jax.random.randint(jax.random.fold_in(own, 2), (rows, 1), 0, top)
    return jnp.take_along_axis(listing, (jnp.arange(top)[None, :] + offset_by) % top, axis=1)


def portions_of(number_of, total, reach, skew, full):
    portions = [(1 << 20) // math.isqrt(grade ** skew) + 1 for grade in range(1, number_of + 1)]
    largest = reach if full else min(reach, max(-(-total // number_of), total * portions[0] // sum(portions)))
    least = 1 if total - largest >= number_of - 1 else 0
    holding, rest = [largest] + [least] * (number_of - 1), total - largest - least * (number_of - 1)
    while rest > 0:
        candidates = [i for i in range(1, number_of) if holding[i] < largest] or [i for i in range(1, number_of) if holding[i] < reach]
        pool, left = sum([portions[i] for i in candidates]), rest
        for i in candidates:
            extra = min(reach - holding[i], max(1, left * portions[i] // pool), rest)
            holding[i] = holding[i] + extra
            rest = rest - extra
    return np.array(holding)


def bell_draw(key, extent, spread, reach, cuts=(), kind=jnp.bfloat16):
    entries = jax.random.normal(key, extent, jnp.float32) * spread
    if len(cuts) > 0:
        entries = steps_of(key, extent, cuts, -0.22, 0.18) * entries
    return jnp.clip(entries, min=-reach, max=reach).astype(kind)


def setup_inputs(seed: int = 0) -> dict:
    arg_keys = jax.random.split(jax.random.key(seed), 23)
    hidden_in = bell_draw(arg_keys[0], (SEQS, D), 1.0, 6.0, ((0, 8), (1, 4)))
    state_in = bell_draw(arg_keys[1], (SEQS, H, DK, DV), 0.09, 0.6, ((0, 8), (1, 4)), jnp.float32)
    attn_gain = jnp.clip(1.0 + 0.18 * jax.random.normal(arg_keys[2], (D,), jnp.float32), 0.1, 1.9)
    w_query = bell_draw(arg_keys[3], (D, H * DK), D ** -0.5, 0.125, ((1, 4),))
    w_key = bell_draw(arg_keys[4], (D, H * DK), D ** -0.5, 0.125, ((1, 4),))
    w_value = bell_draw(arg_keys[5], (D, H * DV), D ** -0.5, 0.125, ((1, 4),))
    w_gate = bell_draw(arg_keys[6], (D, H * DV), D ** -0.5, 0.125, ((1, 4),))
    w_beta = bell_draw(arg_keys[7], (D, H), D ** -0.5, 0.125)
    w_decay = bell_draw(arg_keys[8], (D, H), D ** -0.5, 0.125)
    decay_scale = jnp.clip(jnp.exp(jax.random.uniform(arg_keys[9], (H,), jnp.float32, math.log(0.05), math.log(3.0))), 0.05, 3.0)
    head_gain = jnp.clip(1.0 + 0.18 * jax.random.normal(arg_keys[10], (DV,), jnp.float32), 0.1, 1.9)
    w_output = bell_draw(arg_keys[11], (H * DV, D), (H * DV) ** -0.5, 0.1875, ((1, 4),))
    ffn_gain = jnp.clip(1.0 + 0.18 * jax.random.normal(arg_keys[12], (D,), jnp.float32), 0.1, 1.9)
    expert_ids_keys = jax.random.split(jax.random.fold_in(arg_keys[13], 1), SEQS // SEQ_DEV)
    expert_ids_turns = jax.random.permutation(jax.random.fold_in(arg_keys[13], 3), SEQS // SEQ_DEV)
    expert_ids = jax.vmap(lambda own, number: deal_out(jax.random.fold_in(arg_keys[13], 2), own, number, SEQ_DEV, EXPERTS, TOP, CAP, 2))(expert_ids_keys, expert_ids_turns).reshape((SEQS, TOP))
    route_weight = jnp.clip(jnp.exp(math.log(1.0) - 1.609438 * jax.random.uniform(arg_keys[14], (SEQS, TOP), jnp.float32) ** steps_of(arg_keys[14], (SEQS, TOP), ((0, 8),), -0.2, 0.2)), 0.2, 1.0)
    expert_gate = bell_draw(arg_keys[15], (EXPERTS, D, FE), D ** -0.5, 0.125, ((0, 8), (2, 4)))
    expert_up = bell_draw(arg_keys[16], (EXPERTS, D, FE), D ** -0.5, 0.125, ((0, 8), (2, 4)))
    expert_down = bell_draw(arg_keys[17], (EXPERTS, FE, D), FE ** -0.5, 0.109375, ((0, 8), (1, 4)))
    dense_gate = bell_draw(arg_keys[18], (D, FFD), D ** -0.5, 0.125, ((1, 8),))
    dense_up = bell_draw(arg_keys[19], (D, FFD), D ** -0.5, 0.125, ((1, 8),))
    dense_down = bell_draw(arg_keys[20], (FFD, D), FFD ** -0.5, 0.09375, ((0, 8),))
    dense_mix = bell_draw(arg_keys[21], (D,), 1.5, 6.0, ((0, 4),), jnp.float32)
    return dict(hidden_in=hidden_in, state_in=state_in, attn_gain=attn_gain, w_query=w_query, w_key=w_key, w_value=w_value, w_gate=w_gate, w_beta=w_beta, w_decay=w_decay, decay_scale=decay_scale, head_gain=head_gain, w_output=w_output, ffn_gain=ffn_gain, expert_ids=expert_ids, route_weight=route_weight, expert_gate=expert_gate, expert_up=expert_up, expert_down=expert_down, dense_gate=dense_gate, dense_up=dense_up, dense_down=dense_down, dense_mix=dense_mix)


EPS = 1e-06

def root_norm(values, scale_vec):
    wide = values.astype(jnp.float32)
    return wide * lax.rsqrt(lax.optimization_barrier(jnp.mean(wide * wide, axis=-1, keepdims=True)) + EPS) * scale_vec.astype(jnp.float32)

def unit_norm(values):
    return values * lax.rsqrt(lax.optimization_barrier(jnp.sum(values * values, axis=-1, keepdims=True)) + EPS)

def slot_table(expert_ids, count):
    flat = expert_ids.reshape(-1)
    onehot = (flat[:, None] == jnp.arange(count, dtype=jnp.int32)[None, :]).astype(jnp.int32)
    before = jnp.cumsum(onehot, axis=0) - onehot
    return lax.optimization_barrier(jnp.sum(before * onehot, axis=1)).reshape(expert_ids.shape)

def delta_update(old_state, key_rows, value_rows, beta_rate, decay_rate):
    recalled = jnp.einsum('shk,shkv->shv', key_rows, old_state, precision=lax.Precision.HIGHEST)
    erased = old_state - beta_rate[..., None, None] * key_rows[..., :, None] * recalled[..., None, :]
    written = beta_rate[..., None, None] * key_rows[..., :, None] * value_rows[..., None, :]
    return decay_rate[..., None, None] * erased + written

def head_output(new_state, queries, gate_rows, head_gain):
    read = jnp.einsum('shk,shkv->shv', queries, new_state, precision=lax.Precision.HIGHEST)
    return (root_norm(read, head_gain) * jax.nn.silu(gate_rows)).astype(jnp.bfloat16)

def reference(hidden_in, state_in, attn_gain, w_query, w_key, w_value, w_gate, w_beta, w_decay, decay_scale, head_gain, w_output, ffn_gain, expert_ids, route_weight, expert_gate, expert_up, expert_down, dense_gate, dense_up, dense_down, dense_mix):
    seqs = hidden_in.shape[0]
    normed = root_norm(hidden_in, attn_gain).astype(jnp.bfloat16)
    queries = unit_norm(jnp.dot(normed, w_query, preferred_element_type=jnp.float32).reshape(seqs, H, DK)) * DK ** (-0.5)
    key_rows = unit_norm(jnp.dot(normed, w_key, preferred_element_type=jnp.float32).reshape(seqs, H, DK))
    value_rows = jnp.dot(normed, w_value, preferred_element_type=jnp.float32).reshape(seqs, H, DV)
    gate_rows = jnp.dot(normed, w_gate, preferred_element_type=jnp.float32).reshape(seqs, H, DV)
    beta_rate = jax.nn.sigmoid(jnp.dot(normed, w_beta, preferred_element_type=jnp.float32))
    decay_logit = jnp.dot(normed, w_decay, preferred_element_type=jnp.float32)
    decay_rate = jnp.exp(-decay_scale[None, :] * jax.nn.softplus(decay_logit))
    new_state = delta_update(state_in, key_rows, value_rows, beta_rate, decay_rate)
    heads_out = head_output(new_state, queries, gate_rows, head_gain).reshape(seqs, H * DV)
    mixed = (hidden_in.astype(jnp.float32) + jnp.dot(heads_out, w_output, preferred_element_type=jnp.float32)).astype(jnp.bfloat16)
    normed2 = root_norm(mixed, ffn_gain).astype(jnp.bfloat16)
    groups = expert_ids.reshape(N_EP, SEQ_DEV, TOP)
    slots = jax.vmap(lambda group_ids: slot_table(group_ids, EXPERTS))(groups).reshape(seqs, TOP)
    group_index = (jnp.arange(seqs, dtype=jnp.int32) // SEQ_DEV)[:, None]
    place = (group_index * CAP + slots).astype(jnp.int32)
    spread_rows = jnp.broadcast_to(normed2[:, None, :], (seqs, TOP, D))
    buffer = jnp.zeros((EXPERTS, N_EP * CAP, D), jnp.bfloat16).at[expert_ids, place].set(spread_rows)

    def one_expert(operands):
        rows, gate_weight, up_weight, down_weight = operands
        gate_val = jnp.dot(rows, gate_weight, preferred_element_type=jnp.float32)
        up_val = jnp.dot(rows, up_weight, preferred_element_type=jnp.float32)
        inner = (jax.nn.silu(gate_val) * up_val).astype(jnp.bfloat16)
        width = inner.shape[1] // N_TP
        total = jnp.zeros((rows.shape[0], D), jnp.float32)
        for section in range(N_TP):
            term = jnp.dot(inner[:, section * width:(section + 1) * width], down_weight[section * width:(section + 1) * width, :], preferred_element_type=jnp.float32)
            total = total + lax.optimization_barrier(term.astype(jnp.bfloat16)).astype(jnp.float32)
        return total.astype(jnp.bfloat16)
    expert_out = lax.map(one_expert, (buffer, expert_gate, expert_up, expert_down))
    picked = expert_out[expert_ids, place].astype(jnp.float32)
    moe_sum = lax.optimization_barrier(jnp.sum(route_weight[..., None] * picked, axis=1))
    dense_gate_val = jnp.dot(normed2, dense_gate, preferred_element_type=jnp.float32)
    dense_up_val = jnp.dot(normed2, dense_up, preferred_element_type=jnp.float32)
    dense_hidden = (jax.nn.silu(dense_gate_val) * dense_up_val).astype(jnp.bfloat16)
    dense_out = jnp.dot(dense_hidden, dense_down, preferred_element_type=jnp.float32)
    result = (mixed.astype(jnp.float32) + moe_sum + jax.nn.sigmoid(dense_mix)[None, :] * dense_out).astype(jnp.bfloat16)
    return (result, new_state)
```

```python
import functools

import jax
import jax.numpy as jnp
from jax import lax
from jax.experimental import pallas as pl
from jax.experimental.pallas import tpu as pltpu
from jax.sharding import PartitionSpec as P

EPS = 1e-06


def root_norm(values, scale_vec):
    wide = values.astype(jnp.float32)
    return wide * lax.rsqrt(jnp.mean(wide * wide, axis=-1, keepdims=True) + EPS) * scale_vec


def unit_norm(values):
    return values * lax.rsqrt(jnp.sum(values * values, axis=-1, keepdims=True) + EPS)


def slot_table(expert_ids, count):
    flat = expert_ids.reshape(-1)
    onehot = (flat[:, None] == jnp.arange(count, dtype=jnp.int32)[None, :]).astype(jnp.int32)
    before = jnp.cumsum(onehot, axis=0) - onehot
    return jnp.sum(before * onehot, axis=1).reshape(expert_ids.shape)


def delta_update(old_state, key_rows, value_rows, beta_rate, decay_rate):
    recalled = jnp.einsum("shk,shkv->shv", key_rows, old_state, precision=lax.Precision.HIGHEST)
    erased = (
        old_state - beta_rate[..., None, None] * key_rows[..., :, None] * recalled[..., None, :]
    )
    written = beta_rate[..., None, None] * key_rows[..., :, None] * value_rows[..., None, :]
    return decay_rate[..., None, None] * erased + written


def head_output(new_state, queries, gate_rows, head_gain):
    read = jnp.einsum("shk,shkv->shv", queries, new_state, precision=lax.Precision.HIGHEST)
    return (root_norm(read, head_gain) * jax.nn.silu(gate_rows)).astype(jnp.bfloat16)


def per_device(
    hidden_in,
    state_in,
    attn_gain,
    w_query,
    w_key,
    w_value,
    w_gate,
    w_beta,
    w_decay,
    decay_scale,
    head_gain,
    w_output,
    ffn_gain,
    expert_ids,
    route_weight,
    expert_gate,
    expert_up,
    expert_down,
    dense_gate,
    dense_up,
    dense_down,
    dense_mix,
):
    seq_dev = hidden_in.shape[0]
    tp_size = lax.axis_size("tp")
    ep_size = lax.axis_size("ep")
    tp_index = lax.axis_index("tp")
    local_heads = state_in.shape[1]
    key_dim = state_in.shape[2]
    value_dim = state_in.shape[3]
    local_width = hidden_in.shape[1]
    model_width = local_width * tp_size
    full_rows = lax.all_gather(hidden_in, "tp", axis=1, tiled=True)
    normed = root_norm(full_rows, attn_gain).astype(jnp.bfloat16)
    queries = unit_norm(
        jnp.dot(normed, w_query, preferred_element_type=jnp.float32).reshape(
            seq_dev, local_heads, key_dim
        )
    ) * key_dim ** (-0.5)
    key_rows = unit_norm(
        jnp.dot(normed, w_key, preferred_element_type=jnp.float32).reshape(
            seq_dev, local_heads, key_dim
        )
    )
    value_rows = jnp.dot(normed, w_value, preferred_element_type=jnp.float32).reshape(
        seq_dev, local_heads, value_dim
    )
    gate_rows = jnp.dot(normed, w_gate, preferred_element_type=jnp.float32).reshape(
        seq_dev, local_heads, value_dim
    )
    head_start = tp_index * local_heads
    beta_all = jnp.dot(normed, w_beta, preferred_element_type=jnp.float32)
    decay_all = jnp.dot(normed, w_decay, preferred_element_type=jnp.float32)
    beta_rate = jax.nn.sigmoid(lax.dynamic_slice_in_dim(beta_all, head_start, local_heads, 1))
    decay_logit = lax.dynamic_slice_in_dim(decay_all, head_start, local_heads, 1)
    decay_local = lax.dynamic_slice_in_dim(decay_scale, head_start, local_heads, 0)
    decay_rate = jnp.exp(-decay_local[None, :] * jax.nn.softplus(decay_logit))
    new_state = delta_update(state_in, key_rows, value_rows, beta_rate, decay_rate)
    heads_out = head_output(new_state, queries, gate_rows, head_gain).reshape(
        seq_dev, local_heads * value_dim
    )
    all_heads = lax.all_gather(heads_out, "tp", axis=1, tiled=True)
    mixed = (
        hidden_in.astype(jnp.float32)
        + jnp.dot(all_heads, w_output, preferred_element_type=jnp.float32)
    ).astype(jnp.bfloat16)
    block_rows = seq_dev // tp_size
    top_count = expert_ids.shape[1]
    experts_all = expert_gate.shape[0] * ep_size
    capacity = max(2, 2 * seq_dev * top_count // experts_all)
    slots = slot_table(expert_ids, experts_all)
    place = expert_ids * capacity + slots
    columns = jnp.arange(experts_all * capacity, dtype=jnp.int32)
    send_matrix = jnp.sum(
        (place[None, :, :] == columns[:, None, None]).astype(jnp.bfloat16), axis=2
    )
    take_matrix = jnp.sum(
        jnp.where(place[:, :, None] == columns[None, None, :], route_weight[:, :, None], 0.0),
        axis=1,
    )
    mixed_full = lax.all_gather(mixed, "tp", axis=1, tiled=True)
    normed2 = root_norm(mixed_full, ffn_gain).astype(jnp.bfloat16)
    dense_rows = lax.dynamic_slice_in_dim(normed2, tp_index * block_rows, block_rows, 0)
    outgoing = jnp.dot(send_matrix, normed2, preferred_element_type=jnp.float32).astype(
        jnp.bfloat16
    )
    outgoing = outgoing.reshape(experts_all, capacity, model_width)
    rows = lax.all_to_all(outgoing, "ep", split_axis=0, concat_axis=0, tiled=True)
    flat = rows.reshape(-1, rows.shape[2])
    gate_val = jnp.dot(flat, expert_gate[0], preferred_element_type=jnp.float32)
    up_val = jnp.dot(flat, expert_up[0], preferred_element_type=jnp.float32)
    inner = (jax.nn.silu(gate_val) * up_val).astype(jnp.bfloat16)
    partial_out = jnp.dot(inner, expert_down[0], preferred_element_type=jnp.float32).reshape(
        rows.shape
    )
    summed = lax.psum_scatter(
        partial_out.astype(jnp.bfloat16), "tp", scatter_dimension=2, tiled=True
    )
    returned = lax.all_to_all(summed, "ep", split_axis=0, concat_axis=0, tiled=True)
    moe_sum = jnp.dot(
        take_matrix,
        returned.reshape(-1, local_width).astype(jnp.float32),
        precision=lax.Precision.HIGHEST,
    )
    piece = lax.all_gather(dense_rows, "ep", axis=0, tiled=True)
    gate_val = jnp.dot(piece, dense_gate, preferred_element_type=jnp.float32)
    up_val = jnp.dot(piece, dense_up, preferred_element_type=jnp.float32)
    dense_hidden = (jax.nn.silu(gate_val) * up_val).astype(jnp.bfloat16)
    dense_own = lax.psum_scatter(
        jnp.dot(dense_hidden, dense_down, preferred_element_type=jnp.float32).astype(jnp.bfloat16),
        "ep",
        scatter_dimension=0,
        tiled=True,
    ).astype(jnp.float32)
    dense_out = lax.all_to_all(
        dense_own.astype(jnp.bfloat16), "tp", split_axis=1, concat_axis=0, tiled=True
    ).astype(dense_own.dtype)
    result = (
        mixed.astype(jnp.float32) + moe_sum + jax.nn.sigmoid(dense_mix)[None, :] * dense_out
    ).astype(jnp.bfloat16)
    return (result, new_state)


MESH = pl.DeviceIdType.MESH
F32 = jnp.float32
BF16 = jnp.bfloat16
GROUP = 8


def mm(left, right):
    return jnp.dot(left, right, preferred_element_type=F32)


def layer_kernel(
    dims,
    hidden,
    attn_gain,
    w_beta,
    w_decay,
    decay_scale,
    head_gain,
    ffn_gain,
    expert_ids,
    route_weight,
    dense_mix,
    state_hbm,
    wq_hbm,
    wk_hbm,
    wv_hbm,
    wg_hbm,
    wo_hbm,
    eg_hbm,
    eu_hbm,
    ed_hbm,
    dg_hbm,
    du_hbm,
    dd_hbm,
    out,
    st,
    wq,
    wk,
    wv,
    wg,
    wo,
    eg,
    eu,
    ed,
    dg,
    du,
    dd,
    x_all,
    q_s,
    k_s,
    v_s,
    g_s,
    b_s,
    d_s,
    read_s,
    heads_all,
    mixed_all,
    norm_s,
    piece_s,
    moe_rows,
    ids_all,
    dpart_send,
    dpart_recv,
    dfin_send,
    dfin_recv,
    inner_s,
    part_send,
    part_recv,
    own_s,
    pair_send,
    pair_recv,
    ret_send,
    ret_recv,
    load_sem,
    tp_send,
    tp_recv,
    ep_send,
    ep_recv,
    fan_send,
    fan_recv,
):
    n_ep, n_tp, rows, lh, dk, cap = dims
    t = lax.axis_index("tp")
    e = lax.axis_index("ep")
    width = hidden.shape[1]
    block = rows // n_tp
    mate = t + 1 - 2 * lax.rem(t, 2)
    across = lax.rem(t + 2, n_tp)
    corner = lax.rem(mate + 2, n_tp)

    pairs = (
        (wq_hbm, wq),
        (wk_hbm, wk),
        (wv_hbm, wv),
        (wg_hbm, wg),
        (state_hbm, st),
        (wo_hbm, wo),
        (dg_hbm, dg),
        (du_hbm, du),
        (dd_hbm, dd),
        (eg_hbm.at[0], eg),
        (eu_hbm.at[0], eu),
        (ed_hbm.at[0], ed),
    )
    loads = [
        pltpu.make_async_copy(src, dst, load_sem.at[i]) for i, (src, dst) in enumerate(pairs)
    ]
    for load in loads[:5]:
        load.start()

    barrier = pltpu.get_barrier_semaphore()

    def greet_tp(i, carry):
        pl.semaphore_signal(
            barrier, inc=1, device_id={"tp": lax.rem(t + 1 + i, n_tp)}, device_id_type=MESH
        )
        return carry

    def greet_ep(i, carry):
        pl.semaphore_signal(
            barrier, inc=1, device_id={"ep": lax.rem(e + 1 + i, n_ep)}, device_id_type=MESH
        )
        return carry

    lax.fori_loop(0, n_tp - 1, greet_tp, 0)
    lax.fori_loop(0, n_ep - 1, greet_ep, 0)
    x_all[t] = hidden[...]
    ids_all[e] = jnp.zeros(ids_all.shape[1:], F32)
    ids_all[e, 0:2, 0:rows] = expert_ids[...].astype(F32)
    pl.semaphore_wait(barrier, n_tp + n_ep - 2)

    def tp_copy(phase, src, dst, i, peer):
        return pltpu.make_async_remote_copy(
            src_ref=src,
            dst_ref=dst,
            send_sem=tp_send.at[phase, i],
            recv_sem=tp_recv.at[phase, i],
            device_id={"tp": peer},
            device_id_type=MESH,
        )

    def ep_copy(phase, src, dst, i, peer):
        return pltpu.make_async_remote_copy(
            src_ref=src,
            dst_ref=dst,
            send_sem=ep_send.at[phase, i],
            recv_sem=ep_recv.at[phase, i],
            device_id={"ep": peer},
            device_id_type=MESH,
        )

    def exchange(make, phase, source, target, me, count):
        def send(i, carry):
            peer = lax.rem(me + 1 + i, count)
            make(phase, source(peer), target.at[me], i, peer).start()
            return carry

        lax.fori_loop(0, count - 1, send, 0)

    def arrive(make, phase, target, me, count):
        def take(i, carry):
            origin = lax.rem(me + count - 1 - i, count)
            make(phase, target.at[origin], target.at[origin], i, origin).wait_recv()
            return carry

        lax.fori_loop(0, count - 1, take, 0)

    def sent(make, phase, source, target, me, count):
        def leave(i, carry):
            peer = lax.rem(me + 1 + i, count)
            make(phase, source(peer), target.at[me], i, peer).wait_send()
            return carry

        lax.fori_loop(0, count - 1, leave, 0)

    exchange(tp_copy, 0, lambda p: x_all.at[t], x_all, t, n_tp)
    exchange(ep_copy, 0, lambda p: ids_all.at[e], ids_all, e, n_ep)
    for load in loads[5:]:
        load.start()
    arrive(tp_copy, 0, x_all, t, n_tp)

    def full_norm(chunks, gain_ref):
        wide = [chunk.astype(F32) for chunk in chunks]
        total = sum(jnp.sum(v * v, axis=-1, keepdims=True) for v in wide)
        scale = lax.rsqrt(total / (n_tp * width) + EPS)
        return jnp.concatenate(
            [wide[c] * scale * gain_ref[:, c * width : (c + 1) * width] for c in range(n_tp)],
            axis=1,
        )

    normed = full_norm([x_all[c] for c in range(n_tp)], attn_gain).astype(BF16)
    beta_all = lax.dot_general(
        normed, w_beta[...], (((1,), (1,)), ((), ())), preferred_element_type=F32
    )
    decay_all = lax.dot_general(
        normed, w_decay[...], (((1,), (1,)), ((), ())), preferred_element_type=F32
    )
    lane = lax.broadcasted_iota(jnp.int32, beta_all.shape, 1)
    lane_one = lax.broadcasted_iota(jnp.int32, decay_scale.shape, 1)
    for load in loads[:4]:
        load.wait()
    query_all = mm(normed, wq[...])
    key_all = mm(normed, wk[...])
    v_all = mm(normed, wv[...])
    g_all = mm(normed, wg[...])
    for h in range(lh):
        cut = slice(h * dk, (h + 1) * dk)
        head = t * lh + h
        q = query_all[:, cut]
        k = key_all[:, cut]
        q_s[h] = q * lax.rsqrt(jnp.sum(q * q, -1, keepdims=True) + EPS) * dk ** (-0.5)
        k_s[h] = k * lax.rsqrt(jnp.sum(k * k, -1, keepdims=True) + EPS)
        v_s[h] = v_all[:, cut]
        g_s[h] = g_all[:, cut]
        beta = jax.nn.sigmoid(
            jnp.sum(jnp.where(lane == head, beta_all, 0.0), -1, keepdims=True)
        )
        logit = jnp.sum(jnp.where(lane == head, decay_all, 0.0), -1, keepdims=True)
        rate = jnp.sum(jnp.where(lane_one == head, decay_scale[...], 0.0), -1, keepdims=True)
        soft = jnp.maximum(logit, 0.0) + jnp.log1p(jnp.exp(-jnp.abs(logit)))
        b_s[h] = jnp.broadcast_to(beta, (rows, dk))
        d_s[h] = jnp.broadcast_to(jnp.exp(-rate * soft), (rows, dk))

    loads[4].wait()

    def update(g, carry):
        start = pl.multiple_of(g * GROUP, GROUP)
        some = pl.ds(start, GROUP)
        for h in range(lh):
            k8 = k_s[h, some, :]
            q8 = q_s[h, some, :]
            v8 = v_s[h, some, :]
            b8 = b_s[h, some, :]
            d8 = d_s[h, some, :]
            kt = k8.T
            both = jnp.concatenate([k8, q8], axis=0).astype(BF16)
            qk = jnp.sum(q8 * k8, axis=-1, keepdims=True)
            reads = []
            for j in range(GROUP):
                old = st[start + j, h]
                rec = mm(both, old.astype(BF16))
                d = d8[j : j + 1]
                w = b8[j : j + 1] * (v8[j : j + 1] - d * rec[j : j + 1])
                st[start + j, h] = d * old + kt[:, j : j + 1] * w
                reads.append(d * rec[GROUP + j : GROUP + j + 1] + qk[j : j + 1] * w)
            read_s[h, some, :] = jnp.concatenate(reads, axis=0)
        return carry

    lax.fori_loop(0, rows // GROUP, update, 0)

    heads = []
    for h in range(lh):
        read = read_s[h]
        scale = lax.rsqrt(jnp.mean(read * read, -1, keepdims=True) + EPS)
        heads.append(read * scale * head_gain[...] * jax.nn.silu(g_s[h]))
    heads_all[t] = jnp.concatenate(heads, axis=1).astype(BF16)
    exchange(tp_copy, 1, lambda p: heads_all.at[t], heads_all, t, n_tp)

    columns = n_ep * cap
    first = expert_ids[0:1, :]
    second = expert_ids[1:2, :]
    down_e = lax.broadcasted_iota(jnp.int32, (n_ep, rows), 0)
    hot0 = (down_e == first).astype(F32)
    hot1 = (down_e == second).astype(F32)
    later = (
        lax.broadcasted_iota(jnp.int32, (rows, rows), 0)
        < lax.broadcasted_iota(jnp.int32, (rows, rows), 1)
    ).astype(F32)
    later = later.astype(BF16)
    before = mm((hot0 + hot1).astype(BF16), later)
    slot0 = jnp.sum(before * hot0, 0, keepdims=True).astype(jnp.int32)
    slot1 = jnp.sum(before * hot1, 0, keepdims=True).astype(jnp.int32)
    down_c = lax.broadcasted_iota(jnp.int32, (columns, rows), 0)
    at0 = (down_c == first * cap + slot0).astype(F32)
    at1 = (down_c == second * cap + slot1).astype(F32)
    take_matrix = at0 * route_weight[0:1, :] + at1 * route_weight[1:2, :]

    arrive(tp_copy, 1, heads_all, t, n_tp)
    loads[5].wait()
    all_heads = jnp.concatenate([heads_all[c] for c in range(n_tp)], axis=1)
    mixed = (hidden[...].astype(F32) + mm(all_heads, wo[...])).astype(BF16)
    mixed_all[t, e] = mixed
    own_mixed = mixed_all.at[t]
    exchange(ep_copy, 1, lambda p: own_mixed.at[e], own_mixed, e, n_ep)

    def fan(kind, owner, s, peer):
        return pltpu.make_async_remote_copy(
            src_ref=mixed_all.at[owner, s],
            dst_ref=mixed_all.at[owner, s],
            send_sem=fan_send.at[kind, s],
            recv_sem=fan_recv.at[kind, s],
            device_id={"tp": peer},
            device_id_type=MESH,
        )

    fan(1, t, e, across).start()
    fan(0, t, e, mate).start()

    def forward(i, carry):
        s = lax.rem(e + n_ep - 1 - i, n_ep)
        ep_copy(1, own_mixed.at[s], own_mixed.at[s], i, s).wait_recv()
        fan(1, t, s, across).start()
        fan(0, t, s, mate).start()
        return carry

    lax.fori_loop(0, n_ep - 1, forward, 0)

    def relay(i, carry):
        s = lax.rem(e + n_ep - i, n_ep)
        fan(1, across, s, across).wait_recv()
        fan(2, across, s, mate).start()
        return carry

    lax.fori_loop(0, n_ep, relay, 0)
    arrive(ep_copy, 0, ids_all, e, n_ep)
    down_k = lax.broadcasted_iota(jnp.int32, (cap, rows), 0)
    wanted = e.astype(F32)

    def take_group(i, carry):
        s = lax.rem(e + n_ep - i, n_ep)
        hot = (ids_all[s] == wanted).astype(F32)[0:2, 0:rows]
        hot = hot[0:1] + hot[1:2]
        rank = mm(jnp.broadcast_to(hot, (8, rows)).astype(BF16), later)[0:1].astype(jnp.int32)
        pick = ((down_k == rank).astype(F32) * hot).astype(BF16)
        fan(0, mate, s, mate).wait_recv()
        fan(2, corner, s, mate).wait_recv()
        normed2 = full_norm([mixed_all[c, s] for c in range(n_tp)], ffn_gain)
        norm_s[...] = normed2
        piece_s[s] = norm_s[pl.ds(pl.multiple_of(t * block, block), block), :]
        moe_rows[s] = mm(pick, normed2.astype(BF16)).astype(BF16)
        return carry

    lax.fori_loop(0, n_ep, take_group, 0)

    for load in loads[6:9]:
        load.wait()
    piece = piece_s[...].reshape(n_ep * block, n_tp * width).astype(BF16)
    dense_hidden = (jax.nn.silu(mm(piece, dg[...])) * mm(piece, du[...])).astype(BF16)
    dense_cols = min(512, dd.shape[1])

    def dense_down(i, carry):
        cols = pl.ds(pl.multiple_of(i * dense_cols, dense_cols), dense_cols)
        value = mm(dense_hidden, dd[:, cols])
        dpart_send[:, :, cols] = value.reshape(n_ep, block, dense_cols).astype(BF16)
        return carry

    lax.fori_loop(0, dd.shape[1] // dense_cols, dense_down, 0)
    exchange(ep_copy, 2, lambda p: dpart_send.at[p], dpart_recv, e, n_ep)
    dpart_recv[e] = dpart_send[e]

    for load in loads[9:11]:
        load.wait()
    flat = moe_rows[...].reshape(n_ep * cap, n_tp * width)
    hidden_cols = 256

    def expert_inner(i, carry):
        cols = pl.ds(pl.multiple_of(i * hidden_cols, hidden_cols), hidden_cols)
        inner_s[:, cols] = (
            jax.nn.silu(mm(flat, eg[:, cols])) * mm(flat, eu[:, cols])
        ).astype(BF16)
        return carry

    lax.fori_loop(0, eg.shape[1] // hidden_cols, expert_inner, 0)
    loads[11].wait()

    def expert_down(chunk):
        cols = pl.ds(pl.multiple_of(chunk * width, width), width)
        return mm(inner_s[...], ed[:, cols])

    def to_mate(i):
        return pltpu.make_async_remote_copy(
            src_ref=part_send.at[i],
            dst_ref=part_recv.at[i],
            send_sem=tp_send.at[2, i],
            recv_sem=tp_recv.at[2, i],
            device_id={"tp": mate},
            device_id_type=MESH,
        )

    def to_mate_step(i, carry):
        part_send[i] = expert_down(lax.rem(mate + 2 - 2 * i, n_tp)).astype(BF16)
        to_mate(i).start()
        return carry

    lax.fori_loop(0, 2, to_mate_step, 0)
    pair = pltpu.make_async_remote_copy(
        src_ref=pair_send,
        dst_ref=pair_recv,
        send_sem=tp_send.at[3, 0],
        recv_sem=tp_recv.at[3, 0],
        device_id={"tp": across},
        device_id_type=MESH,
    )

    def own_step(i, carry):
        value = expert_down(lax.rem(t + 2 - 2 * i, n_tp))
        to_mate(i).wait_recv()
        own_s[i] = value + part_recv[i].astype(F32)

        @pl.when(i == 0)
        def _():
            pair_send[...] = own_s[0].astype(BF16)
            pair.start()

        return carry

    lax.fori_loop(0, 2, own_step, 0)

    arrive(ep_copy, 2, dpart_recv, e, n_ep)
    dense_own = sum(dpart_recv[c].astype(F32) for c in range(n_ep))
    for c in range(n_tp):
        dfin_send[c] = dense_own[:, c * width : (c + 1) * width].astype(BF16)
    exchange(tp_copy, 4, lambda p: dfin_send.at[p], dfin_recv, t, n_tp)
    dfin_recv[t] = dfin_send[t]

    pair.wait_recv()
    summed = (own_s[1] + pair_recv[...].astype(F32)).astype(BF16)
    ret_send[...] = summed.reshape(ret_send.shape)
    exchange(ep_copy, 3, lambda p: ret_send.at[p], ret_recv, e, n_ep)
    ret_recv[e] = ret_send[e]
    arrive(tp_copy, 4, dfin_recv, t, n_tp)
    dense_out = dfin_recv[...].astype(F32).reshape(rows, width)
    base = mixed.astype(F32) + jax.nn.sigmoid(dense_mix[...]) * dense_out
    high = take_matrix.astype(BF16)
    low = (take_matrix - high.astype(F32)).astype(BF16)
    arrive(ep_copy, 3, ret_recv, e, n_ep)
    returned = ret_recv[...].reshape(columns, width)
    over = (((0,), (0,)), ((), ()))
    moe_sum = lax.dot_general(
        high, returned, over, preferred_element_type=F32
    ) + lax.dot_general(low, returned, over, preferred_element_type=F32)
    out[...] = (base + moe_sum).astype(BF16)

    sent(tp_copy, 0, lambda p: x_all.at[t], x_all, t, n_tp)
    sent(tp_copy, 1, lambda p: heads_all.at[t], heads_all, t, n_tp)
    sent(tp_copy, 4, lambda p: dfin_send.at[p], dfin_recv, t, n_tp)
    sent(ep_copy, 0, lambda p: ids_all.at[e], ids_all, e, n_ep)
    sent(ep_copy, 1, lambda p: own_mixed.at[e], own_mixed, e, n_ep)
    sent(ep_copy, 2, lambda p: dpart_send.at[p], dpart_recv, e, n_ep)
    sent(ep_copy, 3, lambda p: ret_send.at[p], ret_recv, e, n_ep)
    pair.wait_send()

    def sent_mate(i, carry):
        to_mate(i).wait_send()
        return carry

    lax.fori_loop(0, 2, sent_mate, 0)

    def sent_fan(s, carry):
        fan(0, t, s, mate).wait_send()
        fan(1, t, s, across).wait_send()
        fan(2, across, s, mate).wait_send()
        return carry

    lax.fori_loop(0, n_ep, sent_fan, 0)


def store_kernel(res, state, out, state_out, sem):
    copies = [
        pltpu.make_async_copy(res, out, sem.at[0]),
        pltpu.make_async_copy(state, state_out, sem.at[1]),
    ]
    for copy in copies:
        copy.start()
    for copy in copies:
        copy.wait()


def store_outputs(res, state):
    away = pl.BlockSpec(memory_space=pl.ANY)
    return tuple(
        pl.pallas_call(
            store_kernel,
            out_shape=(
                jax.ShapeDtypeStruct(res.shape, res.dtype),
                jax.ShapeDtypeStruct(state.shape, state.dtype),
            ),
            in_specs=[away, away],
            out_specs=(away, away),
            scratch_shapes=[pltpu.SemaphoreType.DMA((2,))],
            compiler_params=pltpu.CompilerParams(vmem_limit_bytes=1024 * 1024),
        )(res, state)
    )


def fused_device(n_ep, n_tp, *args):
    (
        hidden_in,
        state_in,
        attn_gain,
        w_query,
        w_key,
        w_value,
        w_gate,
        w_beta,
        w_decay,
        decay_scale,
        head_gain,
        w_output,
        ffn_gain,
        expert_ids,
        route_weight,
        expert_gate,
        expert_up,
        expert_down,
        dense_gate,
        dense_up,
        dense_down,
        dense_mix,
    ) = args
    rows, width = hidden_in.shape
    lh, dk, dv = state_in.shape[1:]
    cap = max(2, 2 * rows * expert_ids.shape[1] // n_ep)
    block = rows // n_tp
    model = width * n_tp
    vmem = pltpu.VMEM
    whole = pl.BlockSpec(memory_space=pltpu.VMEM)
    away = pl.BlockSpec(memory_space=pl.ANY)
    head_shape = (lh, rows, dk)

    def like(array):
        return vmem(array.shape, array.dtype)

    scratch = [
        like(w_query),
        like(w_key),
        like(w_value),
        like(w_gate),
        like(w_output),
        vmem(expert_gate.shape[1:], BF16),
        vmem(expert_up.shape[1:], BF16),
        vmem(expert_down.shape[1:], BF16),
        like(dense_gate),
        like(dense_up),
        like(dense_down),
        vmem((n_tp, rows, width), BF16),
        *[vmem(head_shape, F32) for _ in range(7)],
        vmem((n_tp, rows, lh * dv), BF16),
        vmem((n_tp, n_ep, rows, width), BF16),
        vmem((rows, model), F32),
        vmem((n_ep, block, model), F32),
        vmem((n_ep, cap, model), BF16),
        vmem((n_ep, 8, 128), F32),
        vmem((n_ep, block, model), BF16),
        vmem((n_ep, block, model), BF16),
        vmem((n_tp, block, width), BF16),
        vmem((n_tp, block, width), BF16),
        vmem((n_ep * cap, expert_gate.shape[2]), BF16),
        vmem((2, n_ep * cap, width), BF16),
        vmem((2, n_ep * cap, width), BF16),
        vmem((2, n_ep * cap, width), F32),
        vmem((n_ep * cap, width), BF16),
        vmem((n_ep * cap, width), BF16),
        vmem((n_ep, cap, width), BF16),
        vmem((n_ep, cap, width), BF16),
        pltpu.SemaphoreType.DMA((12,)),
        pltpu.SemaphoreType.DMA((5, n_tp - 1)),
        pltpu.SemaphoreType.DMA((5, n_tp - 1)),
        pltpu.SemaphoreType.DMA((4, n_ep - 1)),
        pltpu.SemaphoreType.DMA((4, n_ep - 1)),
        pltpu.SemaphoreType.DMA((3, n_ep)),
        pltpu.SemaphoreType.DMA((3, n_ep)),
    ]
    return store_outputs(
        *pl.pallas_call(
            functools.partial(layer_kernel, (n_ep, n_tp, rows, lh, dk, cap)),
            out_shape=(
                pltpu.VMEM(hidden_in.shape, BF16),
                pltpu.VMEM(state_in.shape, F32),
            ),
            in_specs=[whole] * 10 + [away] * 12,
            out_specs=(whole, whole),
            scratch_shapes=scratch,
            compiler_params=pltpu.CompilerParams(
                collective_id=0, has_side_effects=True, vmem_limit_bytes=58 * 1024 * 1024
            ),
        )(
            hidden_in,
            attn_gain.reshape(1, -1),
            w_beta.T,
            w_decay.T,
            decay_scale.reshape(1, -1),
            head_gain.reshape(1, -1),
            ffn_gain.reshape(1, -1),
            expert_ids.T,
            route_weight.T,
            dense_mix.reshape(1, -1),
            state_in,
            w_query,
            w_key,
            w_value,
            w_gate,
            w_output,
            expert_gate,
            expert_up,
            expert_down,
            dense_gate,
            dense_up,
            dense_down,
        )
    )


def device_program(n_ep, n_tp, *args):
    rows, width = args[0].shape
    top = args[13].shape[1]
    cap = max(2, 2 * rows * top // n_ep)
    fits = (
        top == 2
        and n_tp == 4
        and rows <= 128
        and args[15].shape[0] == 1
        and cap % 16 == 0
        and rows % GROUP == 0
        and (rows // n_tp) % 8 == 0
        and width % 128 == 0
        and args[15].shape[2] % 256 == 0
        and n_ep <= 128
    )
    if fits:
        return fused_device(n_ep, n_tp, *args)
    return per_device(*args)


def solution(mesh):
    placed = (
        P("ep", "tp"),
        P("ep", "tp", None, None),
        P(),
        P(None, "tp"),
        P(None, "tp"),
        P(None, "tp"),
        P(None, "tp"),
        P(),
        P(),
        P(),
        P(),
        P(None, "tp"),
        P(),
        P("ep", None),
        P("ep", None),
        P("ep", None, "tp"),
        P("ep", None, "tp"),
        P("ep", "tp", None),
        P(None, "ep"),
        P(None, "ep"),
        P("ep", None),
        P("tp"),
    )
    return jax.shard_map(
        functools.partial(device_program, mesh.shape["ep"], mesh.shape["tp"]),
        mesh=mesh,
        in_specs=placed,
        out_specs=(P("ep", "tp"), P("ep", "tp", None, None)),
        check_vma=False,
    )
```

```python
import functools

import jax
import jax.numpy as jnp
from jax import lax
from jax.experimental import pallas as pl
from jax.experimental.pallas import tpu as pltpu
from jax.sharding import PartitionSpec as P

EPS = 1e-06


def root_norm(values, scale_vec):
    wide = values.astype(jnp.float32)
    return wide * lax.rsqrt(jnp.mean(wide * wide, axis=-1, keepdims=True) + EPS) * scale_vec


def unit_norm(values):
    return values * lax.rsqrt(jnp.sum(values * values, axis=-1, keepdims=True) + EPS)


def slot_table(expert_ids, count):
    flat = expert_ids.reshape(-1)
    onehot = (flat[:, None] == jnp.arange(count, dtype=jnp.int32)[None, :]).astype(jnp.int32)
    before = jnp.cumsum(onehot, axis=0) - onehot
    return jnp.sum(before * onehot, axis=1).reshape(expert_ids.shape)


def delta_update(old_state, key_rows, value_rows, beta_rate, decay_rate):
    recalled = jnp.einsum("shk,shkv->shv", key_rows, old_state, precision=lax.Precision.HIGHEST)
    erased = (
        old_state - beta_rate[..., None, None] * key_rows[..., :, None] * recalled[..., None, :]
    )
    written = beta_rate[..., None, None] * key_rows[..., :, None] * value_rows[..., None, :]
    return decay_rate[..., None, None] * erased + written


def head_output(new_state, queries, gate_rows, head_gain):
    read = jnp.einsum("shk,shkv->shv", queries, new_state, precision=lax.Precision.HIGHEST)
    return (root_norm(read, head_gain) * jax.nn.silu(gate_rows)).astype(jnp.bfloat16)


def per_device(
    hidden_in,
    state_in,
    attn_gain,
    w_query,
    w_key,
    w_value,
    w_gate,
    w_beta,
    w_decay,
    decay_scale,
    head_gain,
    w_output,
    ffn_gain,
    expert_ids,
    route_weight,
    expert_gate,
    expert_up,
    expert_down,
    dense_gate,
    dense_up,
    dense_down,
    dense_mix,
):
    seq_dev = hidden_in.shape[0]
    tp_size = lax.axis_size("tp")
    ep_size = lax.axis_size("ep")
    tp_index = lax.axis_index("tp")
    local_heads = state_in.shape[1]
    key_dim = state_in.shape[2]
    value_dim = state_in.shape[3]
    local_width = hidden_in.shape[1]
    model_width = local_width * tp_size
    full_rows = lax.all_gather(hidden_in, "tp", axis=1, tiled=True)
    normed = root_norm(full_rows, attn_gain).astype(jnp.bfloat16)
    queries = unit_norm(
        jnp.dot(normed, w_query, preferred_element_type=jnp.float32).reshape(
            seq_dev, local_heads, key_dim
        )
    ) * key_dim ** (-0.5)
    key_rows = unit_norm(
        jnp.dot(normed, w_key, preferred_element_type=jnp.float32).reshape(
            seq_dev, local_heads, key_dim
        )
    )
    value_rows = jnp.dot(normed, w_value, preferred_element_type=jnp.float32).reshape(
        seq_dev, local_heads, value_dim
    )
    gate_rows = jnp.dot(normed, w_gate, preferred_element_type=jnp.float32).reshape(
        seq_dev, local_heads, value_dim
    )
    head_start = tp_index * local_heads
    beta_all = jnp.dot(normed, w_beta, preferred_element_type=jnp.float32)
    decay_all = jnp.dot(normed, w_decay, preferred_element_type=jnp.float32)
    beta_rate = jax.nn.sigmoid(lax.dynamic_slice_in_dim(beta_all, head_start, local_heads, 1))
    decay_logit = lax.dynamic_slice_in_dim(decay_all, head_start, local_heads, 1)
    decay_local = lax.dynamic_slice_in_dim(decay_scale, head_start, local_heads, 0)
    decay_rate = jnp.exp(-decay_local[None, :] * jax.nn.softplus(decay_logit))
    new_state = delta_update(state_in, key_rows, value_rows, beta_rate, decay_rate)
    heads_out = head_output(new_state, queries, gate_rows, head_gain).reshape(
        seq_dev, local_heads * value_dim
    )
    all_heads = lax.all_gather(heads_out, "tp", axis=1, tiled=True)
    mixed = (
        hidden_in.astype(jnp.float32)
        + jnp.dot(all_heads, w_output, preferred_element_type=jnp.float32)
    ).astype(jnp.bfloat16)
    block_rows = seq_dev // tp_size
    top_count = expert_ids.shape[1]
    experts_all = expert_gate.shape[0] * ep_size
    capacity = max(2, 2 * seq_dev * top_count // experts_all)
    slots = slot_table(expert_ids, experts_all)
    place = expert_ids * capacity + slots
    columns = jnp.arange(experts_all * capacity, dtype=jnp.int32)
    send_matrix = jnp.sum(
        (place[None, :, :] == columns[:, None, None]).astype(jnp.bfloat16), axis=2
    )
    take_matrix = jnp.sum(
        jnp.where(place[:, :, None] == columns[None, None, :], route_weight[:, :, None], 0.0),
        axis=1,
    )
    mixed_full = lax.all_gather(mixed, "tp", axis=1, tiled=True)
    normed2 = root_norm(mixed_full, ffn_gain).astype(jnp.bfloat16)
    dense_rows = lax.dynamic_slice_in_dim(normed2, tp_index * block_rows, block_rows, 0)
    outgoing = jnp.dot(send_matrix, normed2, preferred_element_type=jnp.float32).astype(
        jnp.bfloat16
    )
    outgoing = outgoing.reshape(experts_all, capacity, model_width)
    rows = lax.all_to_all(outgoing, "ep", split_axis=0, concat_axis=0, tiled=True)
    flat = rows.reshape(-1, rows.shape[2])
    gate_val = jnp.dot(flat, expert_gate[0], preferred_element_type=jnp.float32)
    up_val = jnp.dot(flat, expert_up[0], preferred_element_type=jnp.float32)
    inner = (jax.nn.silu(gate_val) * up_val).astype(jnp.bfloat16)
    partial_out = jnp.dot(inner, expert_down[0], preferred_element_type=jnp.float32).reshape(
        rows.shape
    )
    summed = lax.psum_scatter(
        partial_out.astype(jnp.bfloat16), "tp", scatter_dimension=2, tiled=True
    )
    returned = lax.all_to_all(summed, "ep", split_axis=0, concat_axis=0, tiled=True)
    moe_sum = jnp.dot(
        take_matrix,
        returned.reshape(-1, local_width).astype(jnp.float32),
        precision=lax.Precision.HIGHEST,
    )
    piece = lax.all_gather(dense_rows, "ep", axis=0, tiled=True)
    gate_val = jnp.dot(piece, dense_gate, preferred_element_type=jnp.float32)
    up_val = jnp.dot(piece, dense_up, preferred_element_type=jnp.float32)
    dense_hidden = (jax.nn.silu(gate_val) * up_val).astype(jnp.bfloat16)
    dense_own = lax.psum_scatter(
        jnp.dot(dense_hidden, dense_down, preferred_element_type=jnp.float32).astype(jnp.bfloat16),
        "ep",
        scatter_dimension=0,
        tiled=True,
    ).astype(jnp.float32)
    dense_out = lax.all_to_all(
        dense_own.astype(jnp.bfloat16), "tp", split_axis=1, concat_axis=0, tiled=True
    ).astype(dense_own.dtype)
    result = (
        mixed.astype(jnp.float32) + moe_sum + jax.nn.sigmoid(dense_mix)[None, :] * dense_out
    ).astype(jnp.bfloat16)
    return (result, new_state)


MESH = pl.DeviceIdType.MESH
F32 = jnp.float32
BF16 = jnp.bfloat16
GROUP = 8


def mm(left, right):
    return jnp.dot(left, right, preferred_element_type=F32)


def layer_kernel(
    dims,
    hidden_hbm,
    again_hbm,
    w_beta_hbm,
    w_decay_hbm,
    decay_scale_hbm,
    head_gain_hbm,
    fgain_hbm,
    ids_hbm,
    rweight_hbm,
    dmix_hbm,
    state_hbm,
    wq_hbm,
    wk_hbm,
    wv_hbm,
    wg_hbm,
    wo_hbm,
    eg_hbm,
    eu_hbm,
    ed_hbm,
    dg_hbm,
    du_hbm,
    dd_hbm,
    out,
    st,
    attn_gain,
    w_beta,
    w_decay,
    decay_scale,
    head_gain,
    ffn_gain,
    expert_ids,
    route_weight,
    dense_mix,
    wq,
    wk,
    wv,
    wg,
    wo,
    eg,
    eu,
    ed,
    dg,
    du,
    dd,
    x_all,
    q_s,
    k_s,
    v_s,
    g_s,
    b_s,
    d_s,
    read_s,
    heads_all,
    mixed_all,
    piece_s,
    moe_rows,
    pick_s,
    ids_all,
    dpart_send,
    dpart_recv,
    dfin_send,
    dfin_recv,
    inner_s,
    part_send,
    part_recv,
    own_s,
    pair_send,
    pair_recv,
    ret_send,
    ret_recv,
    small_sem,
    load_sem,
    tp_send,
    tp_recv,
    ep_send,
    ep_recv,
    line_send,
    side_send,
    across_send,
    mate_send,
    block_recv,
    dense_send,
    dense_recv,
    give_recv,
    token,
):
    n_ep, n_tp, rows, lh, dk, cap = dims
    t = lax.axis_index("tp")
    e = lax.axis_index("ep")
    width = x_all.shape[2]
    block = rows // n_tp
    mate = t + 1 - 2 * lax.rem(t, 2)
    across = lax.rem(t + 2, n_tp)
    corner = lax.rem(mate + 2, n_tp)
    last = n_ep // 2 - 1
    z = e // 2
    x = e - 2 * z
    beside = 2 * z + 1 - x
    near = (z, z + 1 - 2 * lax.rem(z, 2), 2 - z // 2, last * (1 - z // 2))
    at_end = z * (last - z) == 0

    smalls = [
        pltpu.make_async_copy(src, dst, small_sem.at[i])
        for i, (src, dst) in enumerate(
            (
                (hidden_hbm, x_all.at[t]),
                (again_hbm, attn_gain),
                (w_beta_hbm, w_beta),
                (w_decay_hbm, w_decay),
                (decay_scale_hbm, decay_scale),
                (ids_hbm, expert_ids),
                (head_gain_hbm, head_gain),
                (fgain_hbm, ffn_gain),
                (rweight_hbm, route_weight),
                (dmix_hbm, dense_mix),
            )
        )
    ]
    pairs = (
        (wq_hbm, wq),
        (wk_hbm, wk),
        (wv_hbm, wv),
        (wg_hbm, wg),
        (state_hbm, st),
        (wo_hbm, wo),
        (dg_hbm, dg),
        (du_hbm, du),
        (dd_hbm, dd),
        (eg_hbm.at[0], eg),
        (eu_hbm.at[0], eu),
        (ed_hbm.at[0], ed),
    )
    loads = [
        pltpu.make_async_copy(src, dst, load_sem.at[i]) for i, (src, dst) in enumerate(pairs)
    ]
    barrier = pltpu.get_barrier_semaphore()

    def greet_tp(i, carry):
        pl.semaphore_signal(
            barrier, inc=1, device_id={"tp": lax.rem(t + 1 + i, n_tp)}, device_id_type=MESH
        )
        return carry

    def greet(sem, place):
        pl.semaphore_signal(sem, inc=1, device_id={"ep": place}, device_id_type=MESH)

    smalls[0].start()
    lax.fori_loop(0, n_tp - 1, greet_tp, 0)
    greet(barrier, beside)

    @pl.when(z > 0)
    def _():
        greet(barrier, e - 2)

    @pl.when(z < last)
    def _():
        greet(barrier, e + 2)

    for load in smalls[1:]:
        load.start()
    for load in loads[:5]:
        load.start()
    smalls[0].wait()

    ends = (z + last - 1) // last + (2 * last - z - 1) // last
    pl.semaphore_wait(barrier, n_tp + ends)

    def tp_copy(phase, src, dst, i, peer):
        return pltpu.make_async_remote_copy(
            src_ref=src,
            dst_ref=dst,
            send_sem=tp_send.at[phase, i],
            recv_sem=tp_recv.at[phase, i],
            device_id={"tp": peer},
            device_id_type=MESH,
        )

    def ep_copy(phase, src, dst, i, peer):
        return pltpu.make_async_remote_copy(
            src_ref=src,
            dst_ref=dst,
            send_sem=ep_send.at[phase, i],
            recv_sem=ep_recv.at[phase, i],
            device_id={"ep": peer},
            device_id_type=MESH,
        )

    def exchange(make, phase, source, target, me, count):
        def send(i, carry):
            peer = lax.rem(me + 1 + i, count)
            make(phase, source(peer), target.at[me], i, peer).start()
            return carry

        lax.fori_loop(0, count - 1, send, 0)

    def arrive(make, phase, target, me, count):
        def take(i, carry):
            origin = lax.rem(me + count - 1 - i, count)
            make(phase, target.at[origin], target.at[origin], i, origin).wait_recv()
            return carry

        lax.fori_loop(0, count - 1, take, 0)

    def sent(make, phase, source, target, me, count):
        def leave(i, carry):
            peer = lax.rem(me + 1 + i, count)
            make(phase, source(peer), target.at[me], i, peer).wait_send()
            return carry

        lax.fori_loop(0, count - 1, leave, 0)

    def tp_move(phase, buffer, owner, peer, kind):
        return pltpu.make_async_remote_copy(
            src_ref=buffer.at[owner],
            dst_ref=buffer.at[owner],
            send_sem=tp_send.at[phase, kind],
            recv_sem=tp_recv.at[phase, kind],
            device_id={"tp": peer},
            device_id_type=MESH,
        )

    others = (mate, across, corner)

    def tp_share(phase, buffer):
        for kind in (1, 2, 0):
            tp_move(phase, buffer, t, others[kind], kind).start()

    def tp_take(phase, buffer, kind):
        tp_move(phase, buffer, others[kind], others[kind], kind).wait_recv()

    def tp_left(phase, buffer):
        for kind in range(3):
            tp_move(phase, buffer, t, others[kind], kind).wait_send()

    tp_share(0, x_all)
    for load in loads[5:]:
        load.start()

    @pl.when(z == 1)
    def _():
        greet(token.at[0], e + 2)

    @pl.when(z == last - 1)
    def _():
        greet(token.at[1], e - 2)

    for load in smalls[1:]:
        load.wait()
    for load in loads[:4]:
        load.wait()
    ids_all[e] = jnp.zeros(ids_all.shape[1:], F32)
    ids_all[e, 0:2, 0:rows] = expert_ids[...].astype(F32)

    def project(owner):
        cols = pl.ds(pl.multiple_of(owner * width, width), width)
        wide = x_all[owner].astype(F32)
        total = jnp.sum(wide * wide, axis=-1, keepdims=True)
        part = (wide * attn_gain[:, cols]).astype(BF16)
        over = (((1,), (1,)), ((), ()))
        return (
            total,
            mm(part, wq[cols, :]),
            mm(part, wk[cols, :]),
            mm(part, wv[cols, :]),
            mm(part, wg[cols, :]),
            lax.dot_general(part, w_beta[:, cols], over, preferred_element_type=F32),
            lax.dot_general(part, w_decay[:, cols], over, preferred_element_type=F32),
        )

    def plus(left, right):
        return tuple(a + b for a, b in zip(left, right))

    sums = project(t)
    tp_take(0, x_all, 0)
    sums = plus(sums, project(mate))
    tp_take(0, x_all, 1)
    sums = plus(sums, project(across))
    tp_take(0, x_all, 2)
    sums = plus(sums, project(corner))

    @pl.when(z == 2)
    def _():
        pl.semaphore_wait(token.at[0], 1)
        greet(token.at[0], e + 2)

    @pl.when(z == last - 2)
    def _():
        pl.semaphore_wait(token.at[1], 1)
        greet(token.at[1], e - 2)

    scale = lax.rsqrt(sums[0] / (n_tp * width) + EPS)
    query_all, key_all, v_all, g_all, beta_all, decay_all = [v * scale for v in sums[1:]]
    lane = lax.broadcasted_iota(jnp.int32, beta_all.shape, 1)
    lane_one = lax.broadcasted_iota(jnp.int32, decay_scale.shape, 1)
    for h in range(lh):
        cut = slice(h * dk, (h + 1) * dk)
        head = t * lh + h
        q = query_all[:, cut]
        k = key_all[:, cut]
        q_s[h] = q * lax.rsqrt(jnp.sum(q * q, -1, keepdims=True) + EPS) * dk ** (-0.5)
        k_s[h] = k * lax.rsqrt(jnp.sum(k * k, -1, keepdims=True) + EPS)
        v_s[h] = v_all[:, cut]
        g_s[h] = g_all[:, cut]
        beta = jax.nn.sigmoid(
            jnp.sum(jnp.where(lane == head, beta_all, 0.0), -1, keepdims=True)
        )
        logit = jnp.sum(jnp.where(lane == head, decay_all, 0.0), -1, keepdims=True)
        rate = jnp.sum(jnp.where(lane_one == head, decay_scale[...], 0.0), -1, keepdims=True)
        soft = jnp.maximum(logit, 0.0) + jnp.log1p(jnp.exp(-jnp.abs(logit)))
        b_s[h] = jnp.broadcast_to(beta, (rows, dk))
        d_s[h] = jnp.broadcast_to(jnp.exp(-rate * soft), (rows, dk))

    loads[4].wait()

    sub = lax.broadcasted_iota(jnp.int32, (GROUP, dk), 0)

    def recall(g, carry):
        start = pl.multiple_of(g * GROUP, GROUP)
        some = pl.ds(start, GROUP)
        for h in range(lh):
            k8 = k_s[h, some, :]
            q8 = q_s[h, some, :]
            d8 = d_s[h, some, :]
            both = jnp.concatenate([k8, q8], axis=0).astype(BF16)
            rec_k = jnp.zeros((GROUP, dk), F32)
            rec_q = jnp.zeros((GROUP, dk), F32)
            for j in range(0, GROUP, 2):
                two = jnp.concatenate([st[start + j, h], st[start + j + 1, h]], axis=1)
                rec = mm(both, two.astype(BF16))
                for i in range(2):
                    part = rec[:, i * dk : (i + 1) * dk]
                    rec_k = jnp.where(sub == j + i, part[:GROUP], rec_k)
                    rec_q = jnp.where(sub == j + i, part[GROUP:], rec_q)
            w8 = b_s[h, some, :] * (v_s[h, some, :] - d8 * rec_k)
            v_s[h, some, :] = w8
            qk = jnp.sum(q8 * k8, axis=-1, keepdims=True)
            read_s[h, some, :] = d8 * rec_q + qk * w8
        return carry

    lax.fori_loop(0, rows // GROUP, recall, 0)

    heads = []
    for h in range(lh):
        read = read_s[h]
        scale = lax.rsqrt(jnp.mean(read * read, -1, keepdims=True) + EPS)
        heads.append(read * scale * head_gain[...] * jax.nn.silu(g_s[h]))
    heads_all[t] = jnp.concatenate(heads, axis=1).astype(BF16)
    tp_share(1, heads_all)

    @pl.when(z == last)
    def _():
        pl.semaphore_wait(token.at[0], 1)

    @pl.when(z == 0)
    def _():
        pl.semaphore_wait(token.at[1], 1)

    greet(token.at[2], beside)

    def rank_one(g, carry):
        start = pl.multiple_of(g * GROUP, GROUP)
        some = pl.ds(start, GROUP)
        for h in range(lh):
            kt = k_s[h, some, :].T
            w8 = v_s[h, some, :]
            d8 = d_s[h, some, :]
            for j in range(GROUP):
                st[start + j, h] = d8[j : j + 1] * st[start + j, h] + kt[:, j : j + 1] * w8[j : j + 1]
        return carry

    groups = rows // GROUP
    lax.fori_loop(0, groups // 2, rank_one, 0)
    pl.semaphore_wait(token.at[2], 1)
    exchange(ep_copy, 0, lambda p: ids_all.at[e], ids_all, e, n_ep)
    lax.fori_loop(groups // 2, groups - 1, rank_one, 0)
    loads[5].wait()
    head_cols = heads_all.shape[2]

    def wo_part(owner):
        return mm(heads_all[owner], wo[pl.ds(pl.multiple_of(owner * head_cols, head_cols), head_cols), :])

    mixed = x_all[t].astype(F32) + wo_part(t)
    tp_take(1, heads_all, 0)
    mixed = mixed + wo_part(mate)
    tp_take(1, heads_all, 1)
    mixed = mixed + wo_part(across)
    tp_take(1, heads_all, 2)
    mixed = (mixed + wo_part(corner)).astype(BF16)
    mixed_all[t, e] = mixed

    def move(owner, s, sem, place):
        return pltpu.make_async_remote_copy(
            src_ref=mixed_all.at[owner, s],
            dst_ref=mixed_all.at[owner, s],
            send_sem=sem,
            recv_sem=block_recv.at[owner, s],
            device_id=place,
            device_id_type=MESH,
        )

    def here(k, side):
        return 2 * near[k] + (x if side == 0 else 1 - x)

    def along(k):
        return move(t, e, line_send.at[k - 1], {"ep": here(k, 0)})

    def far():
        return move(t, e, line_send.at[3], {"ep": here(3, 1)})

    def aside(k):
        return move(t, here(k, 0), side_send.at[k], {"ep": beside})

    def over_y(k, side):
        return move(t, here(k, side), across_send.at[k, side], {"tp": across})

    def to_core(k, side, owner, i):
        return move(owner, here(k, side), mate_send.at[i, k, side], {"tp": mate})

    def spread(k, side):
        over_y(k, side).start()
        to_core(k, side, t, 0).start()

    def got(k, side, owner):
        s = here(k, side)
        move(owner, s, mate_send.at[0, k, side], {"tp": mate}).wait_recv()

    def from_line(k):
        got(k, 0, t)
        if k < 3:
            aside(k).start()
        else:

            @pl.when(jnp.logical_not(at_end))
            def _():
                aside(k).start()

        spread(k, 0)

    def from_side(k):
        got(k, 1, t)
        spread(k, 1)

    def from_across(k, side):
        got(k, side, across)
        to_core(k, side, across, 1).start()

    def take_group(k, side):
        s = here(k, side)
        got(k, side, mate)
        got(k, side, corner)
        pick = pick_s[s].astype(BF16)
        wide = [mm(pick, mixed_all[c, s]) for c in range(n_tp)]
        total = sum(jnp.sum(v * v, axis=-1, keepdims=True) for v in wide)
        scale = lax.rsqrt(total / (n_tp * width) + EPS)
        for c in range(n_tp):
            cols = slice(c * width, (c + 1) * width)
            value = wide[c] * scale * ffn_gain[:, cols]
            moe_rows[2 * k + side, :, cols] = value[:cap].astype(BF16)
            piece_s[2 * k + side, :, cols] = value[cap:]

    along(3).start()

    @pl.when(at_end)
    def _():
        far().start()

    spread(0, 0)
    aside(0).start()
    along(2).start()
    along(1).start()
    lax.fori_loop(groups - 1, groups, rank_one, 0)
    columns = n_ep * cap
    first = expert_ids[0:1, :]
    second = expert_ids[1:2, :]
    down_e = lax.broadcasted_iota(jnp.int32, (n_ep, rows), 0)
    hot0 = (down_e == first).astype(F32)
    hot1 = (down_e == second).astype(F32)
    later = (
        lax.broadcasted_iota(jnp.int32, (rows, rows), 0)
        < lax.broadcasted_iota(jnp.int32, (rows, rows), 1)
    ).astype(F32)
    later = later.astype(BF16)
    before = mm((hot0 + hot1).astype(BF16), later)
    slot0 = jnp.sum(before * hot0, 0, keepdims=True).astype(jnp.int32)
    slot1 = jnp.sum(before * hot1, 0, keepdims=True).astype(jnp.int32)
    down_c = lax.broadcasted_iota(jnp.int32, (columns, rows), 0)
    at0 = (down_c == first * cap + slot0).astype(F32)
    at1 = (down_c == second * cap + slot1).astype(F32)
    take_matrix = at0 * route_weight[0:1, :] + at1 * route_weight[1:2, :]

    from_line(1)
    from_side(0)
    from_across(0, 0)
    from_line(2)
    from_line(3)
    arrive(ep_copy, 0, ids_all, e, n_ep)
    wanted = e.astype(F32)
    hot = (ids_all[:, 0, 0:rows] == wanted).astype(F32) + (
        ids_all[:, 1, 0:rows] == wanted
    ).astype(F32)
    rank = mm(hot.astype(BF16), later).astype(jnp.int32)
    down_k = lax.broadcasted_iota(jnp.int32, (cap, rows), 0)
    down_b = lax.broadcasted_iota(jnp.int32, (block, rows), 0)
    along_b = lax.broadcasted_iota(jnp.int32, (block, rows), 1)
    mine = (along_b == down_b + t * block).astype(F32)
    for s in range(n_ep):
        pick_s[s, :cap, :] = (down_k == rank[s : s + 1]).astype(F32) * hot[s : s + 1]
        pick_s[s, cap:, :] = mine
    from_side(1)
    from_across(1, 0)
    from_across(0, 1)
    from_side(2)
    from_side(3)
    take_group(0, 0)
    from_across(2, 0)
    from_across(3, 0)
    from_across(1, 1)
    take_group(1, 0)
    from_across(2, 1)
    take_group(0, 1)
    from_across(3, 1)
    take_group(1, 1)
    take_group(2, 0)
    take_group(3, 0)
    take_group(2, 1)
    take_group(3, 1)

    for load in loads[6:9]:
        load.wait()
    piece = piece_s[...].reshape(n_ep * block, n_tp * width).astype(BF16)
    dense_hidden = (jax.nn.silu(mm(piece, dg[...])) * mm(piece, du[...])).astype(BF16)
    half = dd.shape[1] // 2
    places = [(k, side) for k in (3, 2, 1, 0) for side in (1, 0)][:-1]

    def dense_copy(k, side, part):
        cols = pl.ds(part * half, half)
        return pltpu.make_async_remote_copy(
            src_ref=dpart_send.at[2 * k + side, :, cols],
            dst_ref=dpart_recv.at[e, :, cols],
            send_sem=dense_send.at[part, 2 * k + side],
            recv_sem=dense_recv.at[part, e],
            device_id={"ep": here(k, side)},
            device_id_type=MESH,
        )

    def dense_take(k, side, part):
        cols = pl.ds(part * half, half)
        s = here(k, side)
        return pltpu.make_async_remote_copy(
            src_ref=dpart_send.at[2 * k + side, :, cols],
            dst_ref=dpart_recv.at[s, :, cols],
            send_sem=dense_send.at[part, 2 * k + side],
            recv_sem=dense_recv.at[part, s],
            device_id={"ep": s},
            device_id_type=MESH,
        )

    for part in range(2):
        cols = slice(part * half, (part + 1) * half)
        value = mm(dense_hidden, dd[:, cols])
        dpart_send[:, :, cols] = value.reshape(n_ep, block, half).astype(BF16)
        for k, side in places:
            dense_copy(k, side, part).start()
    dpart_recv[e] = dpart_send[0]

    for load in loads[9:11]:
        load.wait()
    flat = moe_rows[...].reshape(n_ep * cap, n_tp * width)
    hidden_cols = 256

    def expert_inner(i, carry):
        cols = pl.ds(pl.multiple_of(i * hidden_cols, hidden_cols), hidden_cols)
        inner_s[:, cols] = (
            jax.nn.silu(mm(flat, eg[:, cols])) * mm(flat, eu[:, cols])
        ).astype(BF16)
        return carry

    lax.fori_loop(0, eg.shape[1] // hidden_cols, expert_inner, 0)
    loads[11].wait()

    def expert_down(chunk):
        cols = pl.ds(pl.multiple_of(chunk * width, width), width)
        return mm(inner_s[...], ed[:, cols])

    def to_mate(i):
        return pltpu.make_async_remote_copy(
            src_ref=part_send.at[i],
            dst_ref=part_recv.at[i],
            send_sem=tp_send.at[2, i],
            recv_sem=tp_recv.at[2, i],
            device_id={"tp": mate},
            device_id_type=MESH,
        )

    def to_mate_step(i, carry):
        part_send[i] = expert_down(lax.rem(mate + 2 - 2 * i, n_tp)).astype(BF16)
        to_mate(i).start()
        return carry

    lax.fori_loop(0, 2, to_mate_step, 0)
    band = n_ep * cap // 2

    def pair(i):
        some = pl.ds((1 - i) * band, band)
        return pltpu.make_async_remote_copy(
            src_ref=pair_send.at[some],
            dst_ref=pair_recv.at[some],
            send_sem=tp_send.at[3, i],
            recv_sem=tp_recv.at[3, i],
            device_id={"tp": across},
            device_id_type=MESH,
        )

    def own_step(i, carry):
        value = expert_down(lax.rem(t + 2 - 2 * i, n_tp))
        to_mate(i).wait_recv()
        own_s[i] = value + part_recv[i].astype(F32)

        @pl.when(i == 0)
        def _():
            pair_send[...] = own_s[0].astype(BF16)
            pair(0).start()
            pair(1).start()

        return carry

    lax.fori_loop(0, 2, own_step, 0)

    tp_left(0, x_all)
    tp_left(1, heads_all)
    sent(ep_copy, 0, lambda p: ids_all.at[e], ids_all, e, n_ep)
    for k in (1, 2, 3):
        along(k).wait_send()
        aside(k - 1).wait_send()

    @pl.when(at_end)
    def _():
        far().wait_send()

    @pl.when(jnp.logical_not(at_end))
    def _():
        aside(3).wait_send()

    for k in range(4):
        for side in range(2):
            over_y(k, side).wait_send()
            to_core(k, side, t, 0).wait_send()
            to_core(k, side, across, 1).wait_send()

    def ret_copy(k, side):
        return pltpu.make_async_remote_copy(
            src_ref=ret_send.at[2 * k + side],
            dst_ref=ret_recv.at[e],
            send_sem=ep_send.at[1, 2 * k + side - 1],
            recv_sem=give_recv.at[e],
            device_id={"ep": here(k, side)},
            device_id_type=MESH,
        )

    def ret_take(k, side):
        s = here(k, side)
        return pltpu.make_async_remote_copy(
            src_ref=ret_send.at[2 * k + side],
            dst_ref=ret_recv.at[s],
            send_sem=ep_send.at[1, 2 * k + side - 1],
            recv_sem=give_recv.at[s],
            device_id={"ep": s},
            device_id_type=MESH,
        )

    for i in range(2):
        pair(i).wait_recv()
        some = slice((1 - i) * band, (2 - i) * band)
        summed = (own_s[1, some] + pair_recv[some].astype(F32)).astype(BF16)
        ret_send[(1 - i) * n_ep // 2 : (2 - i) * n_ep // 2] = summed.reshape(
            n_ep // 2, cap, width
        )
        for k, side in places:
            if k // 2 == 1 - i:
                ret_copy(k, side).start()
    ret_recv[e] = ret_send[0]
    for part in range(2):
        for k, side in places[::-1]:
            dense_take(k, side, part).wait_recv()
    dense_own = sum(dpart_recv[c].astype(F32) for c in range(n_ep))
    for c in range(n_tp):
        dfin_send[c] = dense_own[:, c * width : (c + 1) * width].astype(BF16)
    exchange(tp_copy, 4, lambda p: dfin_send.at[p], dfin_recv, t, n_tp)
    dfin_recv[t] = dfin_send[t]

    arrive(tp_copy, 4, dfin_recv, t, n_tp)
    dense_out = dfin_recv[...].astype(F32).reshape(rows, width)
    base = mixed.astype(F32) + jax.nn.sigmoid(dense_mix[...]) * dense_out
    high = take_matrix.astype(BF16)
    low = (take_matrix - high.astype(F32)).astype(BF16)
    sent(tp_copy, 4, lambda p: dfin_send.at[p], dfin_recv, t, n_tp)
    for k, side in places:
        for part in range(2):
            dense_copy(k, side, part).wait_send()
    pair(0).wait_send()
    pair(1).wait_send()

    def sent_mate(i, carry):
        to_mate(i).wait_send()
        return carry

    lax.fori_loop(0, 2, sent_mate, 0)
    for k, side in places[::-1]:
        ret_take(k, side).wait_recv()
    returned = ret_recv[...].reshape(columns, width)
    over = (((0,), (0,)), ((), ()))
    moe_sum = lax.dot_general(
        high, returned, over, preferred_element_type=F32
    ) + lax.dot_general(low, returned, over, preferred_element_type=F32)
    out[...] = (base + moe_sum).astype(BF16)
    for k, side in places:
        ret_copy(k, side).wait_send()


def store_kernel(res, state, out, state_out, sem):
    copies = [
        pltpu.make_async_copy(res, out, sem.at[0]),
        pltpu.make_async_copy(state, state_out, sem.at[1]),
    ]
    for copy in copies:
        copy.start()
    for copy in copies:
        copy.wait()


def store_outputs(res, state):
    away = pl.BlockSpec(memory_space=pl.ANY)
    return tuple(
        pl.pallas_call(
            store_kernel,
            out_shape=(
                jax.ShapeDtypeStruct(res.shape, res.dtype),
                jax.ShapeDtypeStruct(state.shape, state.dtype),
            ),
            in_specs=[away, away],
            out_specs=(away, away),
            scratch_shapes=[pltpu.SemaphoreType.DMA((2,))],
            compiler_params=pltpu.CompilerParams(vmem_limit_bytes=1024 * 1024),
        )(res, state)
    )


def fused_device(n_ep, n_tp, *args):
    (
        hidden_in,
        state_in,
        attn_gain,
        w_query,
        w_key,
        w_value,
        w_gate,
        w_beta,
        w_decay,
        decay_scale,
        head_gain,
        w_output,
        ffn_gain,
        expert_ids,
        route_weight,
        expert_gate,
        expert_up,
        expert_down,
        dense_gate,
        dense_up,
        dense_down,
        dense_mix,
    ) = args
    rows, width = hidden_in.shape
    lh, dk, dv = state_in.shape[1:]
    cap = max(2, 2 * rows * expert_ids.shape[1] // n_ep)
    block = rows // n_tp
    model = width * n_tp
    vmem = pltpu.VMEM
    whole = pl.BlockSpec(memory_space=pltpu.VMEM)
    away = pl.BlockSpec(memory_space=pl.ANY)
    head_shape = (lh, rows, dk)

    def like(array):
        return vmem(array.shape, array.dtype)

    scratch = [
        vmem((1, model), F32),
        vmem(w_beta.shape[::-1], BF16),
        vmem(w_decay.shape[::-1], BF16),
        vmem((1, decay_scale.shape[0]), F32),
        vmem((1, head_gain.shape[0]), F32),
        vmem((1, model), F32),
        vmem(expert_ids.shape[::-1], expert_ids.dtype),
        vmem(route_weight.shape[::-1], F32),
        vmem((1, dense_mix.shape[0]), F32),
        like(w_query),
        like(w_key),
        like(w_value),
        like(w_gate),
        like(w_output),
        vmem(expert_gate.shape[1:], BF16),
        vmem(expert_up.shape[1:], BF16),
        vmem(expert_down.shape[1:], BF16),
        like(dense_gate),
        like(dense_up),
        like(dense_down),
        vmem((n_tp, rows, width), BF16),
        *[vmem(head_shape, F32) for _ in range(7)],
        vmem((n_tp, rows, lh * dv), BF16),
        vmem((n_tp, n_ep, rows, width), BF16),
        vmem((n_ep, block, model), F32),
        vmem((n_ep, cap, model), BF16),
        vmem((n_ep, cap + block, rows), F32),
        vmem((n_ep, 8, 128), F32),
        vmem((n_ep, block, model), BF16),
        vmem((n_ep, block, model), BF16),
        vmem((n_tp, block, width), BF16),
        vmem((n_tp, block, width), BF16),
        vmem((n_ep * cap, expert_gate.shape[2]), BF16),
        vmem((2, n_ep * cap, width), BF16),
        vmem((2, n_ep * cap, width), BF16),
        vmem((2, n_ep * cap, width), F32),
        vmem((n_ep * cap, width), BF16),
        vmem((n_ep * cap, width), BF16),
        vmem((n_ep, cap, width), BF16),
        vmem((n_ep, cap, width), BF16),
        pltpu.SemaphoreType.DMA((10,)),
        pltpu.SemaphoreType.DMA((12,)),
        pltpu.SemaphoreType.DMA((5, n_tp - 1)),
        pltpu.SemaphoreType.DMA((5, n_tp - 1)),
        pltpu.SemaphoreType.DMA((4, n_ep - 1)),
        pltpu.SemaphoreType.DMA((4, n_ep - 1)),
        pltpu.SemaphoreType.DMA((4,)),
        pltpu.SemaphoreType.DMA((4,)),
        pltpu.SemaphoreType.DMA((4, 2)),
        pltpu.SemaphoreType.DMA((2, 4, 2)),
        pltpu.SemaphoreType.DMA((n_tp, n_ep)),
        pltpu.SemaphoreType.DMA((2, n_ep)),
        pltpu.SemaphoreType.DMA((2, n_ep)),
        pltpu.SemaphoreType.DMA((n_ep,)),
        pltpu.SemaphoreType.REGULAR((3,)),
    ]
    return store_outputs(
        *pl.pallas_call(
            functools.partial(layer_kernel, (n_ep, n_tp, rows, lh, dk, cap)),
            out_shape=(
                pltpu.VMEM(hidden_in.shape, BF16),
                pltpu.VMEM(state_in.shape, F32),
            ),
            in_specs=[away] * 22,
            out_specs=(whole, whole),
            scratch_shapes=scratch,
            compiler_params=pltpu.CompilerParams(
                collective_id=0, has_side_effects=True, vmem_limit_bytes=58 * 1024 * 1024
            ),
        )(
            hidden_in,
            attn_gain.reshape(1, -1),
            w_beta.T,
            w_decay.T,
            decay_scale.reshape(1, -1),
            head_gain.reshape(1, -1),
            ffn_gain.reshape(1, -1),
            expert_ids.T,
            route_weight.T,
            dense_mix.reshape(1, -1),
            state_in,
            w_query,
            w_key,
            w_value,
            w_gate,
            w_output,
            expert_gate,
            expert_up,
            expert_down,
            dense_gate,
            dense_up,
            dense_down,
        )
    )


def device_program(n_ep, n_tp, *args):
    rows, width = args[0].shape
    top = args[13].shape[1]
    cap = max(2, 2 * rows * top // n_ep)
    fits = (
        top == 2
        and n_tp == 4
        and rows <= 128
        and args[15].shape[0] == 1
        and cap % 16 == 0
        and rows % GROUP == 0
        and (rows // n_tp) % 8 == 0
        and width % 128 == 0
        and args[15].shape[2] % 256 == 0
        and n_ep == 8
    )
    if fits:
        return fused_device(n_ep, n_tp, *args)
    return per_device(*args)


def solution(mesh):
    placed = (
        P("ep", "tp"),
        P("ep", "tp", None, None),
        P(),
        P(None, "tp"),
        P(None, "tp"),
        P(None, "tp"),
        P(None, "tp"),
        P(),
        P(),
        P(),
        P(),
        P(None, "tp"),
        P(),
        P("ep", None),
        P("ep", None),
        P("ep", None, "tp"),
        P("ep", None, "tp"),
        P("ep", "tp", None),
        P(None, "ep"),
        P(None, "ep"),
        P("ep", None),
        P("tp"),
    )
    return jax.shard_map(
        functools.partial(device_program, mesh.shape["ep"], mesh.shape["tp"]),
        mesh=mesh,
        in_specs=placed,
        out_specs=(P("ep", "tp"), P("ep", "tp", None, None)),
        check_vma=False,
    )
```
